256 devices in a mesh: grp: 2 (over y), ep: 32 (over z, core), tp: 4 (over x).
Axes of the slice: x: 4, y: 2, z: 16, core: 2. Of those that a mesh axis runs over, the one named last changes fastest.
The devices are a block of a 4x16x16 slice.
Arguments:
- queries: bfloat16 [8192, 1024], P(('grp', 'ep'), 'tp'), parts along dimension 0, may hold values from -6 to 6
- context_lookup_vectors: bfloat16 [8192, 1024], P(('grp', 'ep'), 'tp'), parts along dimension 0, may hold values from -6 to 6
- values: bfloat16 [8192, 1024], P(('grp', 'ep'), 'tp'), parts along dimension 0, may hold values from -6 to 6
- key_shift: bfloat16 [8192, 8], P(('grp', 'ep'), 'tp'), parts along dimension 0, may hold values from -12 to 0
- head_gain: float32 [1024], P('tp'), may hold values from 0.1 to 1.9
- moe_rows: bfloat16 [32768, 2048], P(('grp', 'ep', 'tp')), parts along dimension 0, may hold values from -6 to 6
- routes: int32 [32768, 2], P(('grp', 'ep', 'tp')), parts along dimension 0, may hold values from 0 to 31, all different within a row; in each aligned block of 128 rows (0 to 127, 128 to 255, ...) at most 9 rows name the same one
- route_scores: float32 [32768, 2], P(('grp', 'ep', 'tp')), parts along dimension 0, may hold values from -8 to 8
- norm_gain: float32 [2048], replicated, may hold values from 0.1 to 1.9
- w_gate: bfloat16 [32, 2048, 3584], P('ep', None, 'tp'), may hold values from -0.125 to 0.125
- w_up: bfloat16 [32, 2048, 3584], P('ep', None, 'tp'), may hold values from -0.125 to 0.125
- w_down: bfloat16 [32, 3584, 2048], P('ep', 'tp'), may hold values from -0.09375 to 0.09375
Outputs:
- attn_out: bfloat16 [8192, 1024], P(('grp', 'ep'), 'tp'), parts along dimension 0
- moe_out: bfloat16 [32768, 2048], P(('grp', 'ep', 'tp')), parts along dimension 0
The draws below stay inside these ranges and needn't reach their ends.
There are 2 independent parts, one for each index of `grp`. The reference program is written for one: setup_inputs(seed, part) draws one part's arguments, and reference() takes and returns one part's arrays. A program takes and returns all parts, laid end to end along the dimension named above; an argument that names none is the same for every part. Nothing has to cross between parts.
Inputs may be any that keep to these rules, and one draw needn't show every extreme that they name: `routes`: each row names 2 different experts. In the rows of one device no expert is named more than 9 times, and some device names some expert exactly 9 times.
All inputs are finite; a program needn't handle non-finite values.
Results may differ from the reference program's by a relative error of at most 0.013.
Values may be sent and summed in bfloat16 or wider, within the bound.
No kernel may reach another device: no remote copies, remote signals or barrier semaphores. Data moves between devices by JAX's collectives and lax.ppermute only.
A program may use at most 128 MiB of HBM per device.

```python
import math
import jax
import jax.numpy as jnp
import numpy as np
from jax import lax

D = 2048
ATTENTION_HEADS = 8
HEAD_DIM = 128
FF = 3584
TOP = 2
TOK_A = 128
ROWS_B = 128
SEQUENCE_LENGTH = 4096
TOKENS_B = 16384
EXPERTS = 32
CAP = 9
N_EP = 32
N_TP = 4


def draw_key_shift(key, part):
    base_key = jax.random.fold_in(key, 11)
    random_subkeys = jax.random.split(base_key, 7)
    slow_share = 0.5
    slow = jax.random.uniform(random_subkeys[0], (ATTENTION_HEADS,), jnp.float32) < slow_share
    slow_level = jnp.log(0.5 / SEQUENCE_LENGTH)
    fast_level = jnp.log(2.3 / 66.0) + jax.random.uniform(random_subkeys[1], (ATTENTION_HEADS,), jnp.float32, -0.5, 0.5)
    head_tier = jnp.where(slow, slow_level, fast_level)
    block_multiplier = jax.random.uniform(random_subkeys[2], (SEQUENCE_LENGTH // TOK_A, ATTENTION_HEADS), jnp.float32, -0.7, 0.7)
    block_multiplier = jnp.repeat(block_multiplier, TOK_A, axis=0)
    coarse_portion = jax.random.uniform(random_subkeys[3], (SEQUENCE_LENGTH, ATTENTION_HEADS), jnp.float32, -0.7, 0.7)
    leading_flares = jax.random.randint(random_subkeys[4], (2,), 0, SEQUENCE_LENGTH // 2)
    remaining_flares = jax.random.randint(random_subkeys[5], (2,), 0, SEQUENCE_LENGTH)
    flare_index = jnp.concatenate([leading_flares, remaining_flares])
    sequence_position = jnp.arange(SEQUENCE_LENGTH, dtype=jnp.int32)
    flaring_now = jnp.any(sequence_position[:, None] == flare_index[None, :], axis=1)
    flare_level = jax.random.uniform(random_subkeys[6], (SEQUENCE_LENGTH, ATTENTION_HEADS), jnp.float32, -1.8, -0.8)
    displaced_values = jnp.where(flaring_now[:, None], flare_level, head_tier[None, :] + block_multiplier + coarse_portion)
    return displaced_values.astype(jnp.bfloat16)


def steps_of(key, extent, cuts, low, top_value):
    def one(position, blocks):
        steps = jax.random.uniform(jax.random.fold_in(jax.random.fold_in(key, 6), position), (blocks,), jnp.float32, low / len(cuts), top_value / len(cuts))
        return jnp.repeat(jnp.exp(steps), extent[position] // blocks).reshape((-1,) + (1,) * (len(extent) - position - 1))

    factor_of = one(*cuts[0])
    for cut in cuts[1:]:
        factor_of = factor_of * one(*cut)
    return factor_of


def routed_block(rng, own, number, rows, amount, top, limit, skew):
    ranking = jax.random.permutation(rng, amount)
    crowded, common = portions_of(amount, rows * top, limit, skew, True), portions_of(amount, rows * top, limit, skew, False)
    places = jnp.arange(amount)

    def named(lengths, rotation):
        used = int((lengths > 0).sum())
        fixed = max(1, used // 4)
        passed = fixed + (places - fixed + rotation * (used - fixed)) % max(1, amount - fixed)
        return jnp.zeros((amount,), jnp.int32).at[ranking[jnp.where(places < fixed, places, passed)]].set(jnp.asarray(lengths, jnp.int32))

    lengths = jnp.where(number % 4 == 0, named(crowded, number // 4), named(common, number - number // 4 - 1))
    mixed = jax.random.permutation(jax.random.fold_in(own, 3), amount)
    source_of, sink = mixed[0:amount // 2 * 2:2], mixed[1:amount // 2 * 2:2]
    room = jnp.minimum(lengths[source_of] - 1, limit - lengths[sink]) // 2
    room = jnp.where((source_of == ranking[0]) | (sink == ranking[0]) | (lengths[sink] == 0), 0, jnp.maximum(room, 0))
    passed = jax.random.randint(jax.random.fold_in(own, 4), (amount // 2,), 0, 1 << 20) % (room + 1)
    lengths = lengths.at[source_of].add(-passed).at[sink].add(passed)
    labels = jnp.searchsorted(jnp.cumsum(lengths), jnp.arange(rows * top), side="right").astype(jnp.int32)
    listing = labels.reshape(top, rows).T
    listing = listing[jax.random.permutation(jax.random.fold_in(own, 1), rows)]
    rotation = jax.random.randint(jax.random.fold_in(own, 2), (rows, 1), 0, top)
    return jnp.take_along_axis(listing, (jnp.arange(top)[None, :] + rotation) % top, axis=1)


def portions_of(number_of, total, limit, lean, full):
    loads = [(1 << 20) // math.isqrt(rank ** lean) + 1 for rank in range(1, number_of + 1)]
    largest = limit if full else min(limit, max(-(-total // number_of), total * loads[0] // sum(loads)))
    least = 1 if total - largest >= number_of - 1 else 0
    counts, surplus = [largest] + [least] * (number_of - 1), total - largest - least * (number_of - 1)
    while surplus > 0:
        candidates = [i for i in range(1, number_of) if counts[i] < largest] or [i for i in range(1, number_of) if counts[i] < limit]
        whole, remaining = sum([loads[i] for i in candidates]), surplus
        for i in candidates:
            addition = min(limit - counts[i], max(1, remaining * loads[i] // whole), surplus)
            counts[i] = counts[i] + addition
            surplus = surplus - addition
    return np.array(counts)


def centred(stream_key, shape, deviation, most, cuts=(), kind=jnp.bfloat16):
    gain = steps_of(stream_key, shape, cuts, -0.22, 0.18) if cuts else 1.0
    values = jax.random.normal(stream_key, shape, jnp.float32) * deviation * gain
    return jnp.minimum(jnp.maximum(values, -most), most).astype(kind)


def setup_inputs(seed: int = 0, part: int = 0) -> dict:
    key_of = jax.random.split(jax.random.key(seed), 13)
    own_keys = jax.random.split(jax.random.fold_in(key_of[12], part), 13)
    queries = centred(own_keys[0], (SEQUENCE_LENGTH, ATTENTION_HEADS * HEAD_DIM), 1.0, 6.0, ((0, 32), (1, 4)))
    context_lookup_vectors = centred(own_keys[1], (SEQUENCE_LENGTH, ATTENTION_HEADS * HEAD_DIM), 1.0, 6.0, ((0, 32), (1, 4)))
    values = centred(own_keys[2], (SEQUENCE_LENGTH, ATTENTION_HEADS * HEAD_DIM), 1.0, 6.0, ((0, 32), (1, 4)))
    key_shift = draw_key_shift(jax.random.fold_in(jax.random.fold_in(key_of[12], part), 71), part)
    head_gain = jnp.clip(1.0 + 0.18 * jax.random.normal(key_of[4], (ATTENTION_HEADS * HEAD_DIM,), jnp.float32), 0.1, 1.9)
    moe_rows = centred(own_keys[5], (TOKENS_B, D), 1.0, 6.0, ((0, 128),))
    routes_keys = jax.random.split(jax.random.fold_in(own_keys[6], 1), TOKENS_B // ROWS_B)
    routes_turns = jax.random.permutation(jax.random.fold_in(own_keys[6], 3), TOKENS_B // ROWS_B)
    routes = jax.vmap(lambda own, number: routed_block(jax.random.fold_in(own_keys[6], 2), own, number, ROWS_B, EXPERTS, TOP, CAP, 1))(routes_keys, routes_turns).reshape((TOKENS_B, TOP))
    route_scores = centred(own_keys[7], (TOKENS_B, TOP), 1.5, 8.0, ((0, 128),), jnp.float32)
    norm_gain = jnp.clip(1.0 + 0.18 * jax.random.normal(key_of[8], (D,), jnp.float32), 0.1, 1.9)
    w_gate = centred(key_of[9], (EXPERTS, D, FF), D ** -0.5, 0.125, ((0, 32), (2, 4)))
    w_up = centred(key_of[10], (EXPERTS, D, FF), D ** -0.5, 0.125, ((0, 32), (2, 4)))
    w_down = centred(key_of[11], (EXPERTS, FF, D), FF ** -0.5, 0.09375, ((0, 32), (1, 4)))
    return dict(queries=queries, context_lookup_vectors=context_lookup_vectors, values=values, key_shift=key_shift, head_gain=head_gain, moe_rows=moe_rows, routes=routes, route_scores=route_scores, norm_gain=norm_gain, w_gate=w_gate, w_up=w_up, w_down=w_down)


EPS = 1e-06

def attention(queries, context_lookup_vectors, values, key_shift, head_gain):
    total = queries.shape[0]
    block = math.gcd(total, 512)
    query_blocks = queries.reshape(total // block, block, ATTENTION_HEADS, HEAD_DIM).astype(jnp.float32)
    keys_all = context_lookup_vectors.reshape(total, ATTENTION_HEADS, HEAD_DIM).astype(jnp.float32)
    values_all = values.reshape(total, ATTENTION_HEADS, HEAD_DIM).astype(jnp.float32)
    shift_table = key_shift.astype(jnp.float32).T
    key_pos = jnp.arange(total, dtype=jnp.int32)
    scale = 1.0 / math.sqrt(HEAD_DIM)

    def one_block(args):
        query_part, index = args
        score = jnp.einsum('qhd,shd->hqs', query_part, keys_all) * scale + shift_table[:, None, :]
        query_pos = index * block + jnp.arange(block, dtype=jnp.int32)
        causal = key_pos[None, :] < query_pos[:, None]
        log_stay = jnp.where(causal, -jax.nn.softplus(score), 0.0)
        survive = lax.cumsum(log_stay, axis=2, reverse=True) - log_stay
        weight = jnp.where(causal, jnp.exp(jax.nn.log_sigmoid(score) + survive), 0.0).astype(jnp.bfloat16)
        return jnp.einsum('hqs,shd->qhd', weight.astype(jnp.float32), values_all)
    mixed = lax.map(one_block, (query_blocks, jnp.arange(total // block, dtype=jnp.int32)))
    mixed = mixed.reshape(total, ATTENTION_HEADS, HEAD_DIM)
    factor = lax.rsqrt(lax.optimization_barrier(jnp.mean(mixed * mixed, axis=2, keepdims=True)) + EPS)
    normed = mixed * factor * head_gain.astype(jnp.float32).reshape(ATTENTION_HEADS, HEAD_DIM)
    return normed.reshape(total, ATTENTION_HEADS * HEAD_DIM).astype(jnp.bfloat16)

def experts(moe_rows, routes, route_scores, norm_gain, w_gate, w_up, w_down):
    rows_f = moe_rows.astype(jnp.float32)
    factor = lax.rsqrt(lax.optimization_barrier(jnp.mean(rows_f * rows_f, axis=1, keepdims=True)) + EPS)
    normed = (rows_f * factor * norm_gain.astype(jnp.float32)).astype(jnp.bfloat16)
    route_weight = jax.nn.softmax(route_scores.astype(jnp.float32), axis=-1)
    flat = routes.reshape(-1).astype(jnp.int32)
    count = flat.shape[0]
    most = N_EP * N_TP * CAP
    block = FF // N_TP

    def per_expert(expert, results):
        chosen = jnp.nonzero(flat == expert, size=most, fill_value=count)[0].astype(jnp.int32)
        source = jnp.minimum(chosen, count - 1) // TOP
        picked = normed[source]
        gate = jnp.dot(picked, w_gate[expert], preferred_element_type=jnp.float32)
        up = jnp.dot(picked, w_up[expert], preferred_element_type=jnp.float32)
        hidden = (jax.nn.silu(gate) * up).astype(jnp.bfloat16)
        hidden_blocks = hidden.reshape(most, N_TP, block).astype(jnp.float32)
        down_blocks = w_down[expert].reshape(N_TP, block, D).astype(jnp.float32)
        partial_value = jnp.einsum('mtb,tbd->tmd', hidden_blocks, down_blocks).astype(jnp.bfloat16)
        summed = lax.optimization_barrier(jnp.sum(partial_value.astype(jnp.float32), axis=0)).astype(jnp.bfloat16)
        return results.at[chosen].set(summed, mode='drop')
    results = lax.fori_loop(0, EXPERTS, per_expert, jnp.zeros((count, D), jnp.bfloat16))
    gathered = results.reshape(-1, TOP, D).astype(jnp.float32)
    return lax.optimization_barrier(jnp.sum(route_weight[:, :, None] * gathered, axis=1)).astype(jnp.bfloat16)

def reference(queries, context_lookup_vectors, values, key_shift, head_gain, moe_rows, routes, route_scores, norm_gain, w_gate, w_up, w_down):
    attn_out = attention(queries, context_lookup_vectors, values, key_shift, head_gain)
    moe_out = experts(moe_rows, routes, route_scores, norm_gain, w_gate, w_up, w_down)
    return (attn_out, moe_out)
```

```python
import functools
import math

import jax
import jax.numpy as jnp
from jax import lax
from jax.experimental import pallas as pl
from jax.experimental.pallas import tpu as pltpu
from jax.sharding import Mesh
from jax.sharding import PartitionSpec as P


EP = ("ep_0", "ep_1")
GRP_EP = ("grp", "ep_0", "ep_1")
GRP_EP_TP = ("grp", "ep_0", "ep_1", "tp")
EPS = 1e-06
LANES = 128
SUB = 16


def shifted(value, axis, step):
    size = lax.axis_size(axis)
    return lax.ppermute(value, axis, [(i, (i + step) % size) for i in range(size)])


def attention_kernel(where_ref, q_ref, kv_ref, gain_ref, out_ref, *, heads, group):
    index = where_ref[0]
    rows = q_ref.shape[0]
    size = LANES
    scale = 1.0 / math.sqrt(size)
    row_id = lax.broadcasted_iota(jnp.int32, (rows, size), 0)
    lane_id = lax.broadcasted_iota(jnp.int32, (rows, size), 1)
    later = (
        lax.broadcasted_iota(jnp.int32, (size, size), 0)
        > lax.broadcasted_iota(jnp.int32, (size, size), 1)
    ).astype(jnp.bfloat16)
    last = index // group
    contract_last = (((1,), (1,)), ((), ()))

    def step(i, carry):
        first = (last - i) * group
        sums = [carry[2 * h] for h in range(heads)]
        tails = [carry[2 * h + 1] for h in range(heads)]
        for h in range(heads):
            q = q_ref[:, h * size : (h + 1) * size]
            for j in reversed(range(group)):
                b = first + j
                k = kv_ref[b, h * size : (h + 1) * size, :]
                v = kv_ref[b, (heads + h) * size : (heads + h + 1) * size, :]
                shift = kv_ref[b, 2 * heads * size : 2 * heads * size + 8, :].astype(jnp.float32)
                shift = shift[h : h + 1, :]
                score = (
                    lax.dot_general(q, k, contract_last, preferred_element_type=jnp.float32)
                    * scale
                    + shift
                )
                causal = lane_id + (b - index) * size < row_id
                soft = jnp.log1p(jnp.exp(-jnp.abs(score)))
                log_stay = jnp.where(causal, -(jnp.maximum(score, 0.0) + soft), 0.0)
                high = log_stay.astype(jnp.bfloat16)
                low = (log_stay - high.astype(jnp.float32)).astype(jnp.bfloat16)
                inner = jnp.dot(high, later, preferred_element_type=jnp.float32) + jnp.dot(
                    low, later, preferred_element_type=jnp.float32
                )
                log_take = jnp.minimum(score, 0.0) - soft
                weight = jnp.where(causal, jnp.exp(log_take + inner + tails[h]), 0.0)
                sums[h] = sums[h] + jnp.dot(
                    weight.astype(jnp.bfloat16), v, preferred_element_type=jnp.float32
                )
                tails[h] = tails[h] + jnp.sum(log_stay, axis=1, keepdims=True)
        out = []
        for h in range(heads):
            out += [sums[h], tails[h]]
        return tuple(out)

    start = []
    for _ in range(heads):
        start += [jnp.zeros((rows, size), jnp.float32), jnp.zeros((rows, 1), jnp.float32)]
    final = lax.fori_loop(0, last + 1, step, tuple(start))
    for h in range(heads):
        mixed = final[2 * h]
        factor = lax.rsqrt(jnp.mean(mixed * mixed, axis=1, keepdims=True) + EPS)
        gain = gain_ref[:, h * size : (h + 1) * size]
        out_ref[:, h * size : (h + 1) * size] = (mixed * factor * gain).astype(out_ref.dtype)


def packed_context(context_lookup_vectors, values, key_shift):
    heads = key_shift.shape[1]
    parts = [context_lookup_vectors[:, h * LANES : (h + 1) * LANES] for h in range(heads)]
    parts += [values[:, h * LANES : (h + 1) * LANES] for h in range(heads)]
    parts.append(jnp.pad(key_shift.T, ((0, 8 - heads), (0, 0))))
    return jnp.concatenate(parts, axis=0)


def mixer(queries, gathered, head_gain, heads):
    rows, width = queries.shape
    where = lax.axis_index(EP).astype(jnp.int32).reshape(1)
    blocks = lax.axis_size(EP)
    vmem = pl.BlockSpec(memory_space=pltpu.VMEM)
    return pl.pallas_call(
        functools.partial(attention_kernel, heads=heads, group=4),
        out_shape=jax.ShapeDtypeStruct((rows, width), jnp.bfloat16),
        in_specs=[pl.BlockSpec(memory_space=pltpu.SMEM), vmem, vmem, vmem],
        out_specs=vmem,
        compiler_params=pltpu.CompilerParams(vmem_limit_bytes=16 * 1024 * 1024),
        name="mixer",
        cost_estimate=pl.CostEstimate(
            flops=8 * rows * rows * blocks * width,
            bytes_accessed=2 * gathered.size,
            transcendentals=3 * rows * rows * blocks * heads,
        ),
    )(where, queries, gathered.reshape(blocks, -1, LANES), head_gain.reshape(1, width))


def feed_kernel(*refs, count, steps, sizes):
    rows = refs[:count]
    gate_ref, up_ref, down_ref = refs[count : count + 3]
    outs = refs[count + 3 : count + 3 + len(sizes)]
    gate_sum, up_sum, hidden = refs[count + 3 + len(sizes) :]
    i = pl.program_id(0)

    @pl.when(i < steps)
    def _():
        piece = jnp.concatenate([r[...] for r in rows], axis=0) if count > 1 else rows[0][...]
        gate = jnp.dot(piece, gate_ref[0], preferred_element_type=jnp.float32)
        up = jnp.dot(piece, up_ref[0], preferred_element_type=jnp.float32)

        @pl.when(i == 0)
        def _():
            gate_sum[...] = gate
            up_sum[...] = up

        @pl.when((i > 0) & (i < steps - 1))
        def _():
            gate_sum[...] += gate
            up_sum[...] += up

        @pl.when(i == steps - 1)
        def _():
            g = gate_sum[...] + gate
            hidden[...] = (g / (1.0 + jnp.exp(-g)) * (up_sum[...] + up)).astype(hidden.dtype)

    @pl.when(i >= steps)
    def _():
        made = jnp.dot(hidden[...], down_ref[0], preferred_element_type=jnp.float32)
        low = 0
        for out, size in zip(outs, sizes):
            out[...] = made[low : low + size].astype(out.dtype)
            low += size


def feed(pieces, sizes, w_gate, w_up, w_down, steps=4):
    width, units = w_gate.shape[1:]
    counts = tuple(p.shape[0] for p in pieces)
    total = sum(counts)
    count = len(pieces)
    part = width // steps
    return pl.pallas_call(
        functools.partial(feed_kernel, count=count, steps=steps, sizes=sizes),
        grid=(2 * steps,),
        out_shape=[jax.ShapeDtypeStruct((n, width), jnp.bfloat16) for n in sizes],
        in_specs=[pl.BlockSpec((n, part), lambda i: (0, jnp.minimum(i, steps - 1))) for n in counts]
        + [pl.BlockSpec((1, part, units), lambda i: (0, jnp.minimum(i, steps - 1), 0))] * 2
        + [pl.BlockSpec((1, units, part), lambda i: (0, 0, jnp.maximum(i - steps, 0)))],
        out_specs=[
            pl.BlockSpec((n, part), lambda i: (0, jnp.maximum(i - steps, 0))) for n in sizes
        ],
        scratch_shapes=[
            pltpu.VMEM((total, units), jnp.float32),
            pltpu.VMEM((total, units), jnp.float32),
            pltpu.VMEM((total, units), jnp.bfloat16),
        ],
        compiler_params=pltpu.CompilerParams(
            dimension_semantics=("arbitrary",), vmem_limit_bytes=20 * 1024 * 1024
        ),
        name="feed",
        cost_estimate=pl.CostEstimate(
            flops=6 * total * width * units,
            bytes_accessed=6 * width * units + 4 * total * width,
            transcendentals=total * units,
        ),
    )(*pieces, w_gate, w_up, w_down)


def join_kernel(own_ref, a_ref, b_ref, c_ref, d_ref, out_ref, tiles_ref):
    half, _ = a_ref.shape
    for low, first, second in ((0, a_ref, c_ref), (half, b_ref, d_ref)):
        for k in range(SUB):
            cut = slice(k * LANES, (k + 1) * LANES)
            value = (
                own_ref[low : low + half, cut].astype(jnp.float32)
                + first[:, cut].astype(jnp.float32)
                + second[:, cut].astype(jnp.float32)
            )
            tiles_ref[pl.ds(low * SUB + k, half, stride=SUB), :] = value
    out_ref[...] = tiles_ref[...].astype(out_ref.dtype)


def joined(own, before_low, before_high, after_low, after_high):
    count, width = own.shape
    vmem = pl.BlockSpec(memory_space=pltpu.VMEM)
    return pl.pallas_call(
        join_kernel,
        out_shape=jax.ShapeDtypeStruct((count * SUB, LANES), jnp.bfloat16),
        in_specs=[vmem] * 5,
        out_specs=vmem,
        scratch_shapes=[pltpu.VMEM((count * SUB, LANES), jnp.float32)],
        compiler_params=pltpu.CompilerParams(vmem_limit_bytes=12 * 1024 * 1024),
        name="join",
        cost_estimate=pl.CostEstimate(
            flops=1000 * count * width, bytes_accessed=8 * count * width, transcendentals=0
        ),
    )(own, before_low, before_high, after_low, after_high)


def added(*arrays):
    total = arrays[0].astype(jnp.float32)
    for a in arrays[1:]:
        total = total + a.astype(jnp.float32)
    return total.astype(jnp.bfloat16)


def at_experts(own, w_gate, w_up, w_down):
    half = own.shape[0] // 2
    before = shifted(own, "tp", 1)
    after = shifted(own, "tp", -1)
    across_low = shifted(before[:half], "tp", 1)
    across_high = shifted(after[half:], "tp", -1)
    own_part, before_low, before_high, after_low, after_high = feed(
        (own, before, after), (2 * half, half, half, half, half), w_gate, w_up, w_down
    )
    from_before_high = shifted(after_high, "tp", 1)
    from_after_low = shifted(before_low, "tp", -1)
    across_low, across_high, own_part = lax.optimization_barrier(
        (across_low, across_high, own_part)
    )
    low, high = feed((across_low, across_high), (half, half), w_gate, w_up, w_down)
    low = shifted(low, "tp", 1)
    high = shifted(high, "tp", -1)
    from_before_low = shifted(added(after_low, low), "tp", 1)
    from_after_high = shifted(added(before_high, high), "tp", -1)
    return joined(own_part, from_before_low, from_before_high, from_after_low, from_after_high)


def exchanged(tiles, peers):
    tiles = tiles.reshape(peers, -1, SUB, LANES)
    return lax.all_to_all(tiles, EP, 0, 0, tiled=True)


def local(
    queries,
    context_lookup_vectors,
    values,
    key_shift,
    head_gain,
    moe_rows,
    routes,
    route_scores,
    norm_gain,
    w_gate,
    w_up,
    w_down,
):
    rows, width = moe_rows.shape
    top = routes.shape[1]
    heads = key_shift.shape[1]
    peers = lax.axis_size(EP)
    capacity = top * rows // peers + max(1, top * rows // (8 * peers))
    first = (capacity + 1) // 2
    chunks = (first, capacity - first)
    rows_f = moe_rows.astype(jnp.float32)
    factor = lax.rsqrt(jnp.mean(rows_f * rows_f, axis=1, keepdims=True) + EPS)
    normed = (rows_f * factor * norm_gain).astype(jnp.bfloat16)
    route_weight = jax.nn.softmax(route_scores, axis=-1)
    flat = routes.reshape(-1)
    onehot = (flat[:, None] == jnp.arange(peers, dtype=jnp.int32)[None, :]).astype(jnp.int32)
    rank = jnp.sum((jnp.cumsum(onehot, axis=0) - onehot) * onehot, axis=1)
    sent = []
    weights = []
    low = 0
    for size in chunks:
        slot = jnp.where(
            (rank >= low) & (rank < low + size), flat * size + rank - low, -1
        ).reshape(rows, top)
        slots = jnp.arange(peers * size, dtype=jnp.int32)
        placing = jnp.any(slot[None, :, :] == slots[:, None, None], axis=2).astype(jnp.bfloat16)
        sent.append(
            jnp.dot(placing, normed, preferred_element_type=jnp.float32).astype(jnp.bfloat16)
        )
        weights.append(
            jnp.sum(
                jnp.where(slot[:, :, None] == slots[None, None, :], route_weight[:, :, None], 0.0),
                axis=1,
            )
        )
        low += size

    arrived = []
    for s, size in zip(sent, chunks):
        arrived.append(exchanged(s, peers).reshape(peers * size, width))
    context = packed_context(context_lookup_vectors, values, key_shift)
    _, context = lax.optimization_barrier((arrived[0], context))
    gathered = lax.all_gather(context, EP, axis=0, tiled=True)
    attn_out = mixer(queries, gathered, head_gain, heads)
    total = jnp.zeros((rows, width), jnp.float32)
    for a, w, size in zip(arrived, weights, chunks):
        result = at_experts(a, w_gate, w_up, w_down)
        back = exchanged(result, peers).reshape(peers * size, width)
        high = w.astype(jnp.bfloat16)
        rest = (w - high.astype(jnp.float32)).astype(jnp.bfloat16)
        total = (
            total
            + jnp.dot(high, back, preferred_element_type=jnp.float32)
            + jnp.dot(rest, back, preferred_element_type=jnp.float32)
        )
    return (attn_out, total.astype(jnp.bfloat16))


def solution(mesh):
    cores = 2
    chips = mesh.shape["ep"] // cores
    torus = Mesh(
        mesh.devices.reshape(mesh.shape["grp"], chips, cores, mesh.shape["tp"]),
        ("grp", "ep_0", "ep_1", "tp"),
    )
    return jax.shard_map(
        local,
        mesh=torus,
        in_specs=(
            P(GRP_EP, "tp"),
            P(GRP_EP, "tp"),
            P(GRP_EP, "tp"),
            P(GRP_EP, "tp"),
            P("tp"),
            P(GRP_EP_TP, None),
            P(GRP_EP_TP, None),
            P(GRP_EP_TP, None),
            P(),
            P(EP, None, "tp"),
            P(EP, None, "tp"),
            P(EP, "tp", None),
        ),
        out_specs=(P(GRP_EP, "tp"), P(GRP_EP_TP, None)),
        check_vma=False,
    )
```
